32 devices in a mesh: sp: 8 (over z, y), dp: 4 (over x, core).
Axes of the slice: x: 2, y: 2, z: 4, core: 2. Of those that a mesh axis runs over, the one named last changes fastest.
Arguments:
- query_first: bfloat16 [4, 1024, 1024], P('dp', 'sp'), may hold values from -200 to 200
- key_first: bfloat16 [4, 1024, 1024], P('dp', 'sp'), may hold values from -8 to 8
- query_second: bfloat16 [4, 1024, 1024], P('dp', 'sp'), may hold values from -200 to 200
- key_second: bfloat16 [4, 1024, 1024], P('dp', 'sp'), may hold values from -8 to 8
- value_rows: bfloat16 [4, 1024, 2048], P('dp', 'sp'), may hold values from -6 to 6
- mix_lambda: float32 [16], replicated, may hold values from 0.3 to 0.8
- head_gain: float32 [128], replicated, may hold values from 0.1 to 1.9
- residual: bfloat16 [4, 1024, 2048], P('dp', 'sp'), may hold values from -6 to 6
- out_weight: bfloat16 [2048, 2048], replicated, may hold values from -0.125 to 0.125
- norm_gain: float32 [2048], replicated, may hold values from 0.1 to 1.9
- routes: int32 [4, 1024, 4], P('dp', 'sp'), may hold values from 0 to 31, all different within a row; in each aligned block of 128 rows (0 to 127, 128 to 255, ..., all dimensions but the last counted through in order) at most 24 rows name the same one
- route_weights: float32 [4, 1024, 4], P('dp', 'sp'), may hold values from 0.1 to 1
- gate_weight: bfloat16 [32, 2048, 1024], P(('sp', 'dp')), may hold values from -0.375 to 0.375
- up_weight: bfloat16 [32, 2048, 1024], P(('sp', 'dp')), may hold values from -0.375 to 0.375
- down_weight: bfloat16 [32, 1024, 2048], P(('sp', 'dp')), may hold values from -0.046875 to 0.046875
Outputs:
- layer_out: bfloat16 [4, 1024, 2048], P('dp', 'sp')
The draws below stay inside these ranges and needn't reach their ends.
Inputs may be any that keep to these rules, and one draw needn't show every extreme that they name: `routes`: within the rows of one device (aligned blocks of 128 positions of a sequence) no expert is named more than 24 times, a bound that some block reaches.
All inputs are finite; a program needn't handle non-finite values.
Results may differ from the reference program's by a relative error of at most 0.0075.
Values may be sent and summed in bfloat16 or wider, within the bound.
A program may use at most 128 MiB of HBM per device.

```python
import math
import jax
import jax.numpy as jnp
import numpy as np
from jax import lax

D = 2048
H = 16
HD = 64
HV = 128
FF = 1024
TOPK = 4
TOK_DEV = 128
LENGTH = 1024
SEQS = 4
EXPERTS = 32
CAP = 24
N_SP = 8
N_DP = 4


def drawn(key, which):
    shape = (SEQS, LENGTH, H * HD)
    keys = jnp.clip(jax.random.normal(jax.random.fold_in(key, 10 + which), shape, jnp.float32) * 1.3, -8.0, 8.0)
    queries = jnp.clip(jax.random.normal(jax.random.fold_in(key, 20 + which), shape, jnp.float32) * 1.3, -8.0, 8.0)
    return (queries, keys)


def draw_query_first(key, part):
    return drawn(key, 0)[0].astype(jnp.bfloat16)


def draw_key_first(key, part):
    return drawn(key, 0)[1].astype(jnp.bfloat16)


def draw_query_second(key, part):
    return drawn(key, 1)[0].astype(jnp.bfloat16)


def draw_key_second(key, part):
    return drawn(key, 1)[1].astype(jnp.bfloat16)


def block_scale(key, dims, cuts, least, top_value):
    factor_of = 1.0
    for dim, blocks in cuts:
        draws = jax.random.uniform(jax.random.fold_in(jax.random.fold_in(key, 6), dim), (blocks,), jnp.float32, least / len(cuts), top_value / len(cuts))
        factor_of = factor_of * jnp.repeat(jnp.exp(draws), dims[dim] // blocks).reshape((-1,) + (1,) * (len(dims) - 1 - dim))
    return factor_of


def shared_out(own_key, own, number, rows, amount, top, bound, slope):
    ranking = jax.random.permutation(own_key, amount)
    heavy_load, ordinary = load_shares(amount, rows * top, bound, slope, True), load_shares(amount, rows * top, bound, slope, False)
    places = jnp.arange(amount)

    def named(lengths, offset_by):
        used = int((lengths > 0).sum())
        fixed = max(1, used // 4)
        passed = fixed + (places - fixed + offset_by * (used - fixed)) % max(1, amount - fixed)
        return jnp.zeros((amount,), jnp.int32).at[ranking[jnp.where(places < fixed, places, passed)]].set(jnp.asarray(lengths, jnp.int32))

    lengths = jnp.where(number % 4 == 0, named(heavy_load, number // 4), named(ordinary, number - number // 4 - 1))
    mixed = jax.random.permutation(jax.random.fold_in(own, 3), amount)
    giver, sink = mixed[0:amount // 2 * 2:2], mixed[1:amount // 2 * 2:2]
    slack = jnp.minimum(lengths[giver] - 1, bound - lengths[sink]) // 2
    slack = jnp.where((giver == ranking[0]) | (sink == ranking[0]) | (lengths[sink] == 0), 0, jnp.maximum(slack, 0))
    passed = jax.random.randint(jax.random.fold_in(own, 4), (amount // 2,), 0, 1 << 20) % (slack + 1)
    lengths = lengths.at[giver].add(-passed).at[sink].add(passed)
    labels = jnp.searchsorted(jnp.cumsum(lengths), jnp.arange(rows * top), side="right").astype(jnp.int32)
    listing = labels.reshape(top, rows).T
    listing = listing[jax.random.permutation(jax.random.fold_in(own, 1), rows)]
    offset_by = jax.random.randint(jax.random.fold_in(own, 2), (rows, 1), 0, top)
    return jnp.take_along_axis(listing, (jnp.arange(top)[None, :] + offset_by) % top, axis=1)


def load_shares(amount, total, most, skew, full):
    weights = [(1 << 20) // math.isqrt(grade ** skew) + 1 for grade in range(1, amount + 1)]
    largest = most if full else min(most, max(-(-total // amount), total * weights[0] // sum(weights)))
    least = 1 if total - largest >= amount - 1 else 0
    holding, surplus = [largest] + [least] * (amount - 1), total - largest - least * (amount - 1)
    while surplus > 0:
        candidates = [i for i in range(1, amount) if holding[i] < largest] or [i for i in range(1, amount) if holding[i] < most]
        pool, remaining = sum([weights[i] for i in candidates]), surplus
        for i in candidates:
            addition = min(most - holding[i], max(1, remaining * weights[i] // pool), surplus)
            holding[i] = holding[i] + addition
            surplus = surplus - addition
    return np.array(holding)


def bell_draw(rng, extent, deviation, bound, split=(), kind=jnp.bfloat16):
    values = jax.random.normal(rng, extent, jnp.float32) * deviation
    if len(split) > 0:
        values = block_scale(rng, extent, split, -0.22, 0.18) * values
    return jnp.clip(values, min=-bound, max=bound).astype(kind)


def setup_inputs(seed: int = 0) -> dict:
    key_list = jax.random.split(jax.random.key(seed), 16)
    query_first = draw_query_first(jax.random.fold_in(key_list[15], 71), 0)
    key_first = draw_key_first(jax.random.fold_in(key_list[15], 71), 0)
    query_second = draw_query_second(jax.random.fold_in(key_list[15], 71), 0)
    key_second = draw_key_second(jax.random.fold_in(key_list[15], 71), 0)
    value_rows = bell_draw(key_list[4], (SEQS, LENGTH, H * HV), 1.0, 6.0, ((0, 4), (1, 8)))
    mix_lambda = jnp.clip(jax.random.uniform(key_list[5], (H,), jnp.float32, 0.3, 0.8), 0.3, 0.8)
    head_gain = jnp.clip(1.0 + 0.18 * jax.random.normal(key_list[6], (HV,), jnp.float32), 0.1, 1.9)
    residual = bell_draw(key_list[7], (SEQS, LENGTH, D), 1.0, 6.0, ((0, 4), (1, 8)))
    out_weight = bell_draw(key_list[8], (H * HV, D), (H * HV) ** -0.5, 0.125)
    norm_gain = jnp.clip(1.0 + 0.18 * jax.random.normal(key_list[9], (D,), jnp.float32), 0.1, 1.9)
    routes_keys = jax.random.split(jax.random.fold_in(key_list[10], 1), SEQS * LENGTH // TOK_DEV)
    routes_turns = jax.random.permutation(jax.random.fold_in(key_list[10], 3), SEQS * LENGTH // TOK_DEV)
    routes = jax.vmap(lambda own, number: shared_out(jax.random.fold_in(key_list[10], 2), own, number, TOK_DEV, EXPERTS, TOPK, CAP, 2))(routes_keys, routes_turns).reshape((SEQS, LENGTH, TOPK))
    route_weights = jnp.clip(0.1 + 0.9 * jax.random.uniform(key_list[11], (SEQS, LENGTH, TOPK), jnp.float32) ** block_scale(key_list[11], (SEQS, LENGTH, TOPK), ((0, 4), (1, 8)), -0.2, 0.2), 0.1, 1.0)
    gate_weight = bell_draw(key_list[12], (EXPERTS, D, FF), (D // 9) ** -0.5, 0.375, ((0, 32),))
    up_weight = bell_draw(key_list[13], (EXPERTS, D, FF), (D // 9) ** -0.5, 0.375, ((0, 32),))
    down_weight = bell_draw(key_list[14], (EXPERTS, FF, D), (16 * FF) ** -0.5, 0.046875, ((0, 32),))
    return dict(query_first=query_first, key_first=key_first, query_second=query_second, key_second=key_second, value_rows=value_rows, mix_lambda=mix_lambda, head_gain=head_gain, residual=residual, out_weight=out_weight, norm_gain=norm_gain, routes=routes, route_weights=route_weights, gate_weight=gate_weight, up_weight=up_weight, down_weight=down_weight)


def head_attention(operands):
    query_one, key_one, query_two, key_two, value_head, weight_two, head_gain = operands
    length = query_one.shape[0]
    qblock = min(length, max(512, length // 16))
    scale = HD ** (-0.5)
    keypos = jnp.arange(length, dtype=jnp.int32)

    def block(start):
        rows = start * qblock + jnp.arange(qblock, dtype=jnp.int32)
        q_one = lax.dynamic_slice_in_dim(query_one, (start * qblock).astype(jnp.int32), qblock, 0)
        q_two = lax.dynamic_slice_in_dim(query_two, (start * qblock).astype(jnp.int32), qblock, 0)
        score_one = jnp.dot(q_one, key_one.T, preferred_element_type=jnp.float32) * scale
        score_two = jnp.dot(q_two, key_two.T, preferred_element_type=jnp.float32) * scale
        visible = keypos[None, :] <= rows[:, None]
        prob_one = jax.nn.softmax(jnp.where(visible, score_one, -1e+30), axis=-1)
        prob_two = jax.nn.softmax(jnp.where(visible, score_two, -1e+30), axis=-1)
        mixture = (prob_one - weight_two * prob_two).astype(jnp.bfloat16)
        head_raw = jnp.dot(mixture, value_head, preferred_element_type=jnp.float32)
        factor = lax.rsqrt(lax.optimization_barrier(jnp.mean(head_raw * head_raw, axis=-1, keepdims=True)) + 1e-06)
        return (head_raw * factor * head_gain).astype(jnp.bfloat16)
    return lax.map(block, jnp.arange(length // qblock, dtype=jnp.int32)).reshape(length, HV)

def reference(query_first, key_first, query_second, key_second, value_rows, mix_lambda, head_gain, residual, out_weight, norm_gain, routes, route_weights, gate_weight, up_weight, down_weight):

    def by_head(array, width):
        return array.reshape(SEQS, LENGTH, H, width).transpose(0, 2, 1, 3).reshape(SEQS * H, LENGTH, width)
    gains = jnp.broadcast_to(head_gain, (SEQS * H, HV))
    heads = lax.map(head_attention, (by_head(query_first, HD), by_head(key_first, HD), by_head(query_second, HD), by_head(key_second, HD), by_head(value_rows, HV), jnp.tile(mix_lambda, SEQS), gains))
    head_out = heads.reshape(SEQS, H, LENGTH, HV).transpose(0, 2, 1, 3).reshape(SEQS * LENGTH, H * HV)
    attn = jnp.dot(head_out, out_weight, preferred_element_type=jnp.float32)
    mixed = residual.reshape(SEQS * LENGTH, D).astype(jnp.float32) + attn
    normed = (mixed * lax.rsqrt(lax.optimization_barrier(jnp.mean(mixed * mixed, axis=-1, keepdims=True)) + 1e-06) * norm_gain).astype(jnp.bfloat16)
    expert_ids = routes.reshape(-1)
    weights = route_weights.reshape(-1)
    total = expert_ids.shape[0]
    order = jnp.argsort(expert_ids, stable=True).astype(jnp.int32)
    counts = jnp.bincount(expert_ids, length=EXPERTS).astype(jnp.int32)
    starts = (jnp.cumsum(counts) - counts).astype(jnp.int32)
    room = CAP * N_SP * N_DP
    offsets = jnp.arange(room, dtype=jnp.int32)

    def expert_step(acc, operands):
        expert, w_gate, w_up, w_down = operands
        slots = jnp.minimum(starts[expert] + offsets, total - 1)
        valid = offsets < counts[expert]
        picks = order[slots]
        tokens = picks // TOPK
        rows = normed[tokens]
        gate = jnp.dot(rows, w_gate, preferred_element_type=jnp.float32)
        upper = jnp.dot(rows, w_up, preferred_element_type=jnp.float32)
        clamped = jnp.minimum(gate, 7.0)
        hidden = ((jnp.clip(upper, -7.0, 7.0) + 1.0) * clamped * jax.nn.sigmoid(1.702 * clamped)).astype(jnp.bfloat16)
        expert_out = jnp.dot(hidden, w_down, preferred_element_type=jnp.float32).astype(jnp.bfloat16)
        scaled = jnp.where(valid, weights[picks], 0.0)[:, None] * expert_out.astype(jnp.float32)
        return (acc.at[tokens].add(scaled), None)
    routed, _ = lax.scan(expert_step, jnp.zeros((SEQS * LENGTH, D), jnp.float32), (jnp.arange(EXPERTS, dtype=jnp.int32), gate_weight, up_weight, down_weight))
    return (mixed + routed).astype(jnp.bfloat16).reshape(SEQS, LENGTH, D)
```

```python
import functools

import jax
import jax.numpy as jnp
from jax import lax
from jax.experimental import pallas as pl
from jax.experimental.pallas import tpu as pltpu
from jax.sharding import PartitionSpec as P

MESH = pl.DeviceIdType.MESH
VMEM = pltpu.VMEM
F32 = jnp.float32
BF16 = jnp.bfloat16


def vspec(number):
    return [pl.BlockSpec(memory_space=VMEM)] * number


def greet(peers):
    barrier = pltpu.get_barrier_semaphore()
    for peer in peers:
        pl.semaphore_signal(barrier, inc=1, device_id=peer, device_id_type=MESH)
    pl.semaphore_wait(barrier, len(peers))


def remote(src, dst, send_sem, recv_sem, peer):
    return pltpu.make_async_remote_copy(
        src_ref=src, dst_ref=dst, send_sem=send_sem, recv_sem=recv_sem, device_id=peer, device_id_type=MESH
    )


def attention_kernel(
    n, rows, heads_local, hd, hv, sliced,
    lam_ref, gain_ref, q1, k1, q2, k2, vv, meta,
    out_ref, meta_out,
    b_q1, b_k1, b_q2, b_k2, b_v, obuf, prob, mix,
    send_sem, recv_sem, local_sem, osend, orecv,
):
    me, dp = lax.axis_index("sp"), lax.axis_index("dp")
    ins = (k1, k2, q1, q2, vv)
    bufs = (b_k1, b_k2, b_q1, b_q2, b_v)
    peers = [(lax.rem(me + d, n), dp) for d in range(1, n)]
    greet(peers)

    def part(index, j):
        if not sliced[index]:
            return ins[index].at[j]
        width = bufs[index].shape[2]
        return ins[index].at[:, pl.ds(pl.multiple_of(j * width, 128), width)]

    def move(index, d):
        j = lax.rem(me + d, n)
        if index == 5:
            return remote(meta, meta_out.at[me], send_sem.at[5, d], recv_sem.at[5, me], (j, dp))
        return remote(part(index, j), bufs[index].at[me], send_sem.at[index, d], recv_sem.at[index, me], (j, dp))

    order = (0, 2, 1, 3, 4, 5)
    sends = [move(index, d) for index in order for d in range(1, n)]
    for copy in sends:
        copy.start()
    locals_ = [pltpu.make_async_copy(part(i, me), bufs[i].at[me], local_sem.at[i]) for i in range(5)]
    locals_.append(pltpu.make_async_copy(meta, meta_out.at[me], local_sem.at[5]))
    for copy in locals_:
        copy.start()
    for copy in locals_:
        copy.wait()

    def arrived(index):
        for d in range(1, n):
            j = lax.rem(me + d, n)
            if index == 5:
                remote(meta, meta_out.at[j], send_sem.at[5, d], recv_sem.at[5, j], (j, dp)).wait_recv()
            else:
                remote(
                    part(index, j), bufs[index].at[j], send_sem.at[index, d], recv_sem.at[index, j], (j, dp)
                ).wait_recv()

    group = 2 if n % 2 == 0 else 1
    qb = group * rows
    width = heads_local * hd
    lw = heads_local * hv
    lane = lax.broadcasted_iota(jnp.int32, (1, width), 1) // hd
    scale = hd ** (-0.5)
    blocks = [(i * group, (i + 1) * group) for i in reversed(range(n // group))]

    def softs(bq, bk, use):
        for lo, hi in blocks:
            keys = hi * rows
            visible = lax.broadcasted_iota(jnp.int32, (qb, keys), 1) <= lo * rows + lax.broadcasted_iota(
                jnp.int32, (qb, keys), 0
            )
            for h in range(heads_local):
                query = bq[lo:hi].reshape(qb, width)
                query = jnp.where(lane == h, query, jnp.zeros_like(query))
                key = bk[:hi].reshape(keys, width)
                score = lax.dot_general(query, key, (((1,), (1,)), ((), ())), preferred_element_type=F32) * scale
                score = jnp.where(visible, score, -1e30)
                powers = jnp.exp(score - jnp.max(score, axis=-1, keepdims=True))
                use(h, slice(lo * rows, hi * rows), keys, powers, jnp.sum(powers, axis=-1, keepdims=True))

    def first(h, at, keys, powers, total):
        prob[h, at, :keys] = powers * (1.0 / total)

    def second(h, at, keys, powers, total):
        mix[h, at, :keys] = (prob[h, at, :keys] - powers * (lam_ref[h] / total)).astype(BF16)

    arrived(0)
    arrived(2)
    softs(b_q1, b_k1, first)
    arrived(1)
    arrived(3)
    softs(b_q2, b_k2, second)
    arrived(4)
    arrived(5)
    for lo, hi in blocks:
        keys = hi * rows
        for h in range(heads_local):
            value = b_v[:hi, :, h * hv : (h + 1) * hv].reshape(keys, hv)
            raw = jnp.dot(mix[h, lo * rows : hi * rows, :keys], value, preferred_element_type=F32)
            factor = lax.rsqrt(jnp.mean(raw * raw, axis=-1, keepdims=True) + 1e-06)
            done = (raw * factor * gain_ref[...]).astype(BF16)
            obuf[lo:hi, :, h * hv : (h + 1) * hv] = done.reshape(group, rows, hv)
        for j in range(lo, hi):

            @pl.when(j != me)
            def _(j=j):
                remote(
                    obuf.at[j],
                    out_ref.at[:, pl.ds(pl.multiple_of(me * lw, 128), lw)],
                    osend.at[j], orecv.at[me], (j, dp),
                ).start()

    out_ref[:, pl.ds(pl.multiple_of(me * lw, 128), lw)] = obuf[me]
    for copy in sends:
        copy.wait_send()
    for d in range(1, n):
        j = lax.rem(me + d, n)
        back = remote(
            obuf.at[j], out_ref.at[:, pl.ds(pl.multiple_of(j * lw, 128), lw)], osend.at[j], orecv.at[j], (j, dp)
        )
        back.wait_send()
        back.wait_recv()


def attention(n, q1, k1, q2, k2, vv, meta, lam, gain, heads):
    rows = q1.shape[0]
    heads_local = heads // n
    hd = q1.shape[1] // heads
    hv = vv.shape[1] // heads
    arrays, sliced = [], []
    for array, width in ((q1, hd), (k1, hd), (q2, hd), (k2, hd), (vv, hv)):
        w = width * heads_local
        good = w % 128 == 0
        arrays.append(array if good else array.reshape(rows, n, w).transpose(1, 0, 2))
        sliced.append(good)
    order = (1, 3, 0, 2, 4)
    w, lw = hd * heads_local, hv * heads_local
    return pl.pallas_call(
        functools.partial(attention_kernel, n, rows, heads_local, hd, hv, [sliced[i] for i in order]),
        out_shape=(
            jax.ShapeDtypeStruct((rows, n * lw), BF16),
            jax.ShapeDtypeStruct((n,) + meta.shape, F32),
        ),
        in_specs=[pl.BlockSpec(memory_space=pltpu.SMEM)]
        + vspec(1)
        + [pl.BlockSpec(memory_space=pl.ANY)] * 5
        + vspec(1),
        out_specs=tuple(vspec(2)),
        scratch_shapes=[VMEM((n, rows, w), BF16)] * 4
        + [VMEM((n, rows, lw), BF16)] * 2
        + [VMEM((heads_local, n * rows, n * rows), F32), VMEM((heads_local, n * rows, n * rows), BF16)]
        + [
            pltpu.SemaphoreType.DMA((6, n)),
            pltpu.SemaphoreType.DMA((6, n)),
            pltpu.SemaphoreType.DMA((6,)),
            pltpu.SemaphoreType.DMA((n,)),
            pltpu.SemaphoreType.DMA((n,)),
        ],
        compiler_params=pltpu.CompilerParams(
            collective_id=0,
            has_side_effects=True,
            vmem_limit_bytes=58 << 20,
        ),
    )(lam, gain, *arrays, meta)


class Place:
    def __init__(self, outer, inner, ndp):
        self.outer, self.inner, self.ndp = outer, inner, ndp
        self.plane = inner * ndp
        sp, self.dp = lax.axis_index("sp"), lax.axis_index("dp")
        self.z, self.y = sp // inner, lax.rem(sp, inner)
        self.me = self.y * ndp + self.dp

    def along(self, z):
        return (z * self.inner + self.y, self.dp)

    def across(self, p):
        return (self.z * self.inner + p // self.ndp, lax.rem(p, self.ndp))

    def all_peers(self):
        peers = [self.along(lax.rem(self.z + d, self.outer)) for d in range(1, self.outer)]
        return peers + [self.across(lax.rem(self.me + d, self.plane)) for d in range(1, self.plane)]

    def order(self):
        tables = [
            sorted(range(self.outer), key=lambda c: (abs(c - z), c if 2 * z < self.outer else -c))
            for z in range(self.outer)
        ]
        steps = []
        for s in range(self.outer):
            value = jnp.int32(tables[0][s])
            for z in range(1, self.outer):
                value = jnp.where(self.z == z, tables[z][s], value)
            steps.append(value)
        return steps

    def relays(self):
        top = self.outer - 1
        tables = []
        for z in range(self.outer):
            late = lambda c, z=z: c + z if c > z else (top - c) + (top - z)
            tables.append(sorted([c for c in range(self.outer) if c != z], key=late))
        steps = []
        for s in range(top):
            value = jnp.int32(tables[0][s])
            for z in range(1, self.outer):
                value = jnp.where(self.z == z, tables[z][s], value)
            steps.append(value)
        return steps


def moe_kernel(
    outer, inner, ndp, parts, x_ref, pick_ref, weigh_ref, mixed_ref, gate_hbm, up_hbm, down_hbm, out_ref,
    gath, staged, recv, hidden, eout, back, from_below, from_above, partial, mine, gate_w, up_w, down_w,
    wsem, gsend, grecv, psend, precv, bsend, brecv, ssend, srecv, own_sem,
):
    at = Place(outer, inner, ndp)
    z, plane = at.z, at.plane
    block, width = recv.shape[2], recv.shape[3]
    held, _, ff = gate_w.shape
    cap = block // held
    piece = width // parts
    spans = [slice(h * piece, (h + 1) * piece) for h in range(parts)]
    order = at.order()
    edge = (z == 0) | (z == outer - 1)
    greet(at.all_peers())
    loads = [
        pltpu.make_async_copy(a, b, wsem.at[i])
        for i, (a, b) in enumerate(((gate_hbm, gate_w), (up_hbm, up_w), (down_hbm, down_w)))
    ]
    own = pltpu.make_async_copy(x_ref, gath.at[z], own_sem)
    own.start()
    own.wait()

    def slab(ref, c, h):
        return ref.at[c, :, spans[h]]

    def up(c, h):
        return remote(
            slab(gath, c, h), slab(gath, c, h), gsend.at[0, c, h], grecv.at[c, h],
            at.along(jnp.minimum(z + 1, outer - 1)),
        )

    def down(c, h):
        return remote(
            slab(gath, c, h), slab(gath, c, h), gsend.at[1, c, h], grecv.at[c, h],
            at.along(jnp.maximum(z - 1, 0)),
        )

    def other(d):
        return lax.rem(at.me + d, plane)

    def out_to(c, d, h):
        p = other(d)
        return remote(
            staged.at[c, p, :, spans[h]], recv.at[c, at.me, :, spans[h]],
            psend.at[c, p, h], precv.at[c, at.me, h], at.across(p),
        )

    def back_to(c, d, h):
        p = other(d)
        return remote(
            eout.at[c, p, :, spans[h]], back.at[c, at.me, :, spans[h]],
            bsend.at[c, p, h], brecv.at[c, at.me, h], at.across(p),
        )

    def chosen(step):
        c = order[0]
        for i in range(1, outer):
            c = jnp.where(step == i, order[i], c)
        return c

    def hand_on(c, h):
        @pl.when((c <= z) & (z < outer - 1))
        def _():
            up(c, h).start()

        @pl.when((c >= z) & (z > 0))
        def _():
            down(c, h).start()

    def give(c, h):
        rows = gath[c, :, spans[h]]
        for p in range(plane):
            staged[c, p, :, spans[h]] = jnp.dot(
                pick_ref[c, p * block : (p + 1) * block, :], rows, preferred_element_type=F32
            ).astype(BF16)
        for d in range(1, plane):
            out_to(c, d, h).start()
        recv[c, at.me, :, spans[h]] = staged[c, at.me, :, spans[h]]

    def spread(step):
        sides = ((z - step, z >= step), (z + step, z + step < outer))
        for h in range(parts):
            for c, there in sides:

                @pl.when(there)
                def _(c=c, h=h):
                    remote(
                        slab(gath, c, h), slab(gath, c, h), gsend.at[0, c, h], grecv.at[c, h], at.along(c)
                    ).wait_recv()
                    hand_on(c, h)

            for c, there in sides:

                @pl.when(there)
                def _(c=c, h=h):
                    give(c, h)

    def give_back(c, h):
        for d in range(1, plane):
            back_to(c, d, h).start()

    def work(step):
        c = chosen(step)
        for d in range(1, plane):
            p = other(d)
            for h in range(parts):
                remote(
                    staged.at[c, p, :, spans[h]], recv.at[c, p, :, spans[h]],
                    psend.at[c, p, h], precv.at[c, p, h], at.across(p),
                ).wait_recv()

        @pl.when(step == 0)
        def _():
            for load in loads:
                load.wait()

        tile = min(512, ff)
        for e in range(held):
            rows = recv[c, :, e * cap : (e + 1) * cap, :].reshape(plane * cap, width)
            for start in range(0, ff, tile):
                cols = slice(start, start + tile)
                gate = jnp.dot(rows, gate_w[e, :, cols], preferred_element_type=F32)
                upper = jnp.dot(rows, up_w[e, :, cols], preferred_element_type=F32)
                clamped = jnp.minimum(gate, 7.0)
                hidden[e, :, cols] = (
                    (jnp.clip(upper, -7.0, 7.0) + 1.0) * clamped * jax.nn.sigmoid(1.702 * clamped)
                ).astype(BF16)
        tile = min(512, piece)
        for h in range(parts):
            for e in range(held):
                for start in range(h * piece, (h + 1) * piece, tile):
                    cols = slice(start, start + tile)
                    result = jnp.dot(hidden[e], down_w[e, :, cols], preferred_element_type=F32).astype(BF16)
                    eout[c, :, e * cap : (e + 1) * cap, cols] = result.reshape(plane, cap, tile)
            back[c, at.me, :, spans[h]] = eout[c, at.me, :, spans[h]]

            @pl.when((step > 0) & ((step > 1) | jnp.logical_not(edge)))
            def _(h=h):
                give_back(c, h)

    def rise(c, h):
        return remote(
            slab(partial, c, h), slab(from_below, c, h), ssend.at[c, h], srecv.at[0, c, h],
            at.along(jnp.minimum(z + 1, outer - 1)),
        )

    def fall(c, h):
        return remote(
            slab(partial, c, h), slab(from_above, c, h), ssend.at[c, h], srecv.at[1, c, h],
            at.along(jnp.maximum(z - 1, 0)),
        )

    def pass_on(c, h):
        @pl.when(c > z)
        def _():
            rise(c, h).start()

        @pl.when(c < z)
        def _():
            fall(c, h).start()

    def first(c):
        return ((c > z) & (z == 0)) | ((c < z) & (z == outer - 1))

    tile = min(512, piece)

    def collect(step, h):
        c = chosen(step)
        for d in range(1, plane):
            p = other(d)
            remote(
                eout.at[c, p, :, spans[h]], back.at[c, p, :, spans[h]],
                bsend.at[c, p, h], brecv.at[c, p, h], at.across(p),
            ).wait_recv()
        for start in range(h * piece, (h + 1) * piece, tile):
            cols = slice(start, start + tile)
            total = jnp.dot(
                weigh_ref[c], back[c, :, :, cols].reshape(plane * block, tile), preferred_element_type=F32
            )
            mine[c, :, cols] = total
            partial[c, :, cols] = total.astype(BF16)

        @pl.when(first(c))
        def _():
            pass_on(c, h)

    def relay(c, h):
        @pl.when(jnp.logical_not(first(c)))
        def _():
            for side, (here, source) in enumerate(((c > z, from_below), (c < z, from_above))):

                @pl.when(here)
                def _(side=side, source=source):
                    remote(
                        slab(partial, c, h), slab(source, c, h), ssend.at[c, h], srecv.at[side, c, h], at.along(c)
                    ).wait_recv()
                    for start in range(h * piece, (h + 1) * piece, tile):
                        cols = slice(start, start + tile)
                        partial[c, :, cols] = (mine[c, :, cols] + source[c, :, cols].astype(F32)).astype(BF16)

            pass_on(c, h)

    for h in range(parts):
        hand_on(z, h)
    for h in range(parts):
        give(z, h)
    for load in loads:
        load.start()

    def turn(step, carry):
        @pl.when((step > 0) & (step < outer))
        def _():
            spread(step)

        @pl.when((step > 0) & (step <= outer))
        def _():
            work(step - 1)

        return carry

    lax.fori_loop(1, outer + 1, turn, 0)

    @pl.when(edge)
    def _():
        if outer > 1:
            for h in range(parts):
                give_back(order[1], h)

    for h in range(parts):
        give_back(z, h)

    relays = at.relays()
    early = outer - 2 if outer == 4 else 0
    for k in range(outer - 1):
        step = jnp.where(edge, k + 2 if k < outer - 2 else 1, k + 1)
        for h in range(parts):
            collect(step, h)
            if 0 < k <= early:
                relay(relays[k - 1], h)
    for c in relays[early:]:
        for h in range(parts):
            relay(c, h)
    for h in range(parts):
        collect(0, h)
    for h in range(parts):
        @pl.when(z > 0)
        def _(h=h):
            remote(
                slab(partial, z, h), slab(from_below, z, h), ssend.at[z, h], srecv.at[0, z, h],
                at.along(jnp.maximum(z - 1, 0)),
            ).wait_recv()

        @pl.when(z < outer - 1)
        def _(h=h):
            remote(
                slab(partial, z, h), slab(from_above, z, h), ssend.at[z, h], srecv.at[1, z, h],
                at.along(jnp.minimum(z + 1, outer - 1)),
            ).wait_recv()

        for start in range(h * piece, (h + 1) * piece, tile):
            cols = slice(start, start + tile)
            total = mine[z, :, cols] + mixed_ref[:, cols]
            total = total + jnp.where(z > 0, from_below[z, :, cols].astype(F32), 0.0)
            total = total + jnp.where(z < outer - 1, from_above[z, :, cols].astype(F32), 0.0)
            out_ref[:, cols] = total.astype(BF16)

    for step, c in enumerate(order):
        for h in range(parts):

            @pl.when((c <= z) & (z < outer - 1))
            def _(c=c, h=h):
                up(c, h).wait_send()

            @pl.when((c >= z) & (z > 0))
            def _(c=c, h=h):
                down(c, h).wait_send()

            if step > 0:
                rise(c, h).wait_send()
            for d in range(1, plane):
                out_to(c, d, h).wait_send()
                back_to(c, d, h).wait_send()


def moe(outer, inner, ndp, normed, pick, weigh, mixed, gate_weight, up_weight, down_weight):
    plane = inner * ndp
    rows, width = normed.shape
    block = pick.shape[1] // plane
    held, _, ff = gate_weight.shape
    parts = 4 if width % 512 == 0 else 1
    flat = (outer, plane, block, width)
    line = (outer, rows, width)
    dma = pltpu.SemaphoreType.DMA
    return pl.pallas_call(
        functools.partial(moe_kernel, outer, inner, ndp, parts),
        out_shape=jax.ShapeDtypeStruct((rows, width), BF16),
        in_specs=vspec(4) + [pl.BlockSpec(memory_space=pl.ANY)] * 3,
        out_specs=vspec(1)[0],
        scratch_shapes=[
            VMEM(line, BF16),
            VMEM(flat, BF16),
            VMEM(flat, BF16),
            VMEM((held, plane * (block // held), ff), BF16),
            VMEM(flat, BF16),
            VMEM(flat, BF16),
            VMEM(line, BF16),
            VMEM(line, BF16),
            VMEM(line, BF16),
            VMEM(line, F32),
            VMEM(gate_weight.shape, BF16),
            VMEM(up_weight.shape, BF16),
            VMEM(down_weight.shape, BF16),
            dma((3,)),
            dma((2, outer, parts)),
            dma((outer, parts)),
            dma((outer, plane, parts)),
            dma((outer, plane, parts)),
            dma((outer, plane, parts)),
            dma((outer, plane, parts)),
            dma((outer, parts)),
            dma((2, outer, parts)),
            dma,
        ],
        compiler_params=pltpu.CompilerParams(
            collective_id=1, has_side_effects=True, vmem_limit_bytes=48 << 20
        ),
    )(normed, pick, weigh, mixed, gate_weight, up_weight, down_weight)


def on_device(
    query_first,
    key_first,
    query_second,
    key_second,
    value_rows,
    mix_lambda,
    head_gain,
    residual,
    out_weight,
    norm_gain,
    routes,
    route_weights,
    gate_weight,
    up_weight,
    down_weight,
):
    n, ndp = lax.axis_size("sp"), lax.axis_size("dp")
    rows = query_first.shape[1]
    heads = mix_lambda.shape[0]
    topk = routes.shape[2]
    held = gate_weight.shape[0]
    outer = 1
    while outer * outer < n:
        outer *= 2
    inner = n // outer
    plane = inner * ndp
    experts_all = held * n * ndp
    capacity = max(2, 3 * rows * topk // (2 * experts_all))
    capacity = -(-capacity // 8) * 8
    block = held * capacity

    sp = lax.axis_index("sp")
    local = heads // n
    lam = lax.dynamic_slice_in_dim(mix_lambda, sp * local, local)
    meta = jnp.concatenate([routes[0].astype(F32).T, route_weights[0].T], axis=0)
    head_out, metas = attention(
        n, query_first[0], key_first[0], query_second[0], key_second[0], value_rows[0],
        meta, lam, head_gain[None, :], heads,
    )

    line = lax.dynamic_index_in_dim(
        metas.reshape(outer, inner, 2 * topk, rows), lax.rem(sp, inner), 1, keepdims=False
    )
    ids, weights = line[:, :topk].astype(jnp.int32), line[:, topk:]
    mine = (sp // inner) * plane * held + jnp.arange(plane * held, dtype=jnp.int32)
    named = ids[:, :, None, :] == mine[None, None, :, None]
    member = jnp.any(named, axis=1)
    weight_of = jnp.sum(jnp.where(named, weights[:, :, None, :], 0.0), axis=1)
    before = (jnp.arange(rows)[:, None] < jnp.arange(rows)[None, :]).astype(BF16)
    rank = jnp.einsum("cet,tu->ceu", member.astype(BF16), before, preferred_element_type=F32).astype(jnp.int32)
    slot = member[:, :, None, :] & (rank[:, :, None, :] == jnp.arange(capacity, dtype=jnp.int32)[None, None, :, None])
    pick = slot.astype(BF16).reshape(outer, plane * block, rows)
    weigh = jnp.where(slot, weight_of[:, :, None, :], 0.0).astype(BF16).reshape(outer, plane * block, rows)
    weigh = weigh.transpose(0, 2, 1)

    attn = jnp.dot(head_out, out_weight, preferred_element_type=F32)
    mixed = residual[0].astype(F32) + attn
    normed = (
        mixed * lax.rsqrt(jnp.mean(mixed * mixed, axis=-1, keepdims=True) + 1e-06) * norm_gain
    ).astype(BF16)
    return moe(outer, inner, ndp, normed, pick, weigh, mixed, gate_weight, up_weight, down_weight)[None]


def solution(mesh):
    spread = P("dp", "sp", None)
    split = P(("sp", "dp"), None, None)
    return jax.shard_map(
        on_device,
        mesh=mesh,
        in_specs=(spread,) * 5 + (P(), P(), spread, P(), P(), spread, spread) + (split,) * 3,
        out_specs=spread,
        check_vma=False,
    )
```

```python
import functools

import jax
import jax.numpy as jnp
from jax import lax
from jax.experimental import pallas as pl
from jax.experimental.pallas import tpu as pltpu
from jax.sharding import PartitionSpec as P

MESH = pl.DeviceIdType.MESH
VMEM = pltpu.VMEM
F32 = jnp.float32
BF16 = jnp.bfloat16


def vspec(number):
    return [pl.BlockSpec(memory_space=VMEM)] * number


def greet(peers):
    barrier = pltpu.get_barrier_semaphore()
    for peer in peers:
        pl.semaphore_signal(barrier, inc=1, device_id=peer, device_id_type=MESH)


def greeted(peers):
    pl.semaphore_wait(pltpu.get_barrier_semaphore(), len(peers))


def remote(src, dst, send_sem, recv_sem, peer):
    return pltpu.make_async_remote_copy(
        src_ref=src, dst_ref=dst, send_sem=send_sem, recv_sem=recv_sem, device_id=peer, device_id_type=MESH
    )


def attention_kernel(
    n, outer, held, rows, heads_local, hd, hv, sliced,
    lam_ref, gain_ref, routes_ref, rw_ref, res_ref, ngain_ref, q1, k1, q2, k2, vv, out_hbm,
    normed_ref, mixed_ref, pick_ref, weigh_ref, out_w,
    b_q1, b_k1, b_q2, b_k2, b_v, obuf, prob, mix, out_ref, meta, meta_out,
    send_sem, recv_sem, local_sem, osend, orecv, wsem,
):
    me, dp = lax.axis_index("sp"), lax.axis_index("dp")
    topk = routes_ref.shape[0]
    ndp, inner = lax.axis_size("dp"), n // outer
    ins = (k1, k2, q1, q2, vv)
    bufs = (b_k1, b_k2, b_q1, b_q2, b_v)
    z, y = me // inner, lax.rem(me, inner)
    peers = [(lax.rem(me + d, n), dp) for d in range(1, n)]
    for d in range(inner):
        peers += [(z * inner + lax.rem(y + d, inner), lax.rem(dp + e, ndp)) for e in range(1, ndp)]
    greet(peers)
    weights = pltpu.make_async_copy(out_hbm, out_w, wsem)
    weights.start()
    down = lax.broadcasted_iota(jnp.int32, (rows, rows), 0)
    over = lax.broadcasted_iota(jnp.int32, (rows, rows), 1)
    eye = (down == over).astype(BF16)
    meta[:topk] = routes_ref[...].astype(F32)
    meta[topk:] = rw_ref[...]
    greeted(peers)

    def part(index, j):
        if not sliced[index]:
            return ins[index].at[j]
        width = bufs[index].shape[2]
        return ins[index].at[:, pl.ds(pl.multiple_of(j * width, 128), width)]

    def move(index, d):
        j = lax.rem(me + d, n)
        if index == 5:
            return remote(meta, meta_out.at[me], send_sem.at[5, d], recv_sem.at[5, me], (j, dp))
        return remote(part(index, j), bufs[index].at[me], send_sem.at[index, d], recv_sem.at[index, me], (j, dp))

    order = (5, 0, 2, 1, 3, 4)
    sends = [move(index, d) for index in order for d in range(1, n)]
    for copy in sends:
        copy.start()
    locals_ = [pltpu.make_async_copy(part(i, me), bufs[i].at[me], local_sem.at[i]) for i in range(5)]
    meta_out[me] = meta[...]
    for copy in locals_:
        copy.start()
    for copy in locals_:
        copy.wait()

    def arrived(index):
        for d in range(1, n):
            j = lax.rem(me + d, n)
            if index == 5:
                remote(meta, meta_out.at[j], send_sem.at[5, d], recv_sem.at[5, j], (j, dp)).wait_recv()
            else:
                remote(
                    part(index, j), bufs[index].at[j], send_sem.at[index, d], recv_sem.at[index, j], (j, dp)
                ).wait_recv()

    group = 2 if n % 2 == 0 else 1
    qb = group * rows
    width = heads_local * hd
    lw = heads_local * hv
    lane = lax.broadcasted_iota(jnp.int32, (1, width), 1) // hd
    scale = hd ** (-0.5)
    blocks = [(i * group, (i + 1) * group) for i in reversed(range(n // group))]

    def softs(lo, hi):
        keys = hi * rows
        at = slice(lo * rows, hi * rows)
        visible = lax.broadcasted_iota(jnp.int32, (qb, keys), 1) <= lo * rows + lax.broadcasted_iota(
            jnp.int32, (qb, keys), 0
        )
        for h in range(heads_local):
            first = None
            for bq, bk in ((b_q1, b_k1), (b_q2, b_k2)):
                query = bq[lo:hi].reshape(qb, width)
                query = jnp.where(lane == h, query, jnp.zeros_like(query))
                key = bk[:hi].reshape(keys, width)
                score = lax.dot_general(query, key, (((1,), (1,)), ((), ())), preferred_element_type=F32) * scale
                score = jnp.where(visible, score, -1e30)
                powers = jnp.exp(score - jnp.max(score, axis=-1, keepdims=True))
                total = jnp.sum(powers, axis=-1, keepdims=True)
                if first is None:
                    first = True
                    prob[:, :keys] = powers * (1.0 / total)
                else:
                    mix[h, at, :keys] = (
                        prob[:, :keys] - powers * (lam_ref[me * heads_local + h] / total)
                    ).astype(BF16)

    def values(lo, hi):
        keys = hi * rows
        for h in range(heads_local):
            value = b_v[:hi, :, h * hv : (h + 1) * hv].reshape(keys, hv)
            raw = jnp.dot(mix[h, lo * rows : hi * rows, :keys], value, preferred_element_type=F32)
            factor = lax.rsqrt(jnp.mean(raw * raw, axis=-1, keepdims=True) + 1e-06)
            done = (raw * factor * gain_ref[...]).astype(BF16)
            obuf[lo:hi, :, h * hv : (h + 1) * hv] = done.reshape(group, rows, hv)
        for j in range(lo, hi):

            @pl.when(j != me)
            def _(j=j):
                remote(
                    obuf.at[j],
                    out_ref.at[:, pl.ds(pl.multiple_of(me * lw, 128), lw)],
                    osend.at[j], orecv.at[me], (j, dp),
                ).start()

    def attend(blocks):
        for i, (lo, hi) in enumerate(blocks):
            softs(lo, hi)
            if i == 0:
                arrived(4)
            values(lo, hi)

    def tables():
        _, slots, _ = pick_ref.shape
        experts = inner * ndp * held
        cap = slots // experts
        name = (z * experts + lax.broadcasted_iota(jnp.int32, (experts, rows), 0)).astype(F32)
        before = (down < over).astype(BF16)
        count = lax.broadcasted_iota(jnp.int32, (experts, cap, rows), 1).astype(F32)
        for c in range(outer):
            line = meta_out[c * inner + y]
            member = jnp.zeros((experts, rows), F32)
            weight = jnp.zeros((experts, rows), F32)
            for t in range(topk):
                named = line[t : t + 1] == name
                member = jnp.where(named, 1.0, member)
                weight = jnp.where(named, line[topk + t : topk + t + 1], weight)
            rank = jnp.dot(member.astype(BF16), before, preferred_element_type=F32)
            rank = jnp.where(member > 0.0, rank, -1.0)
            slot = rank[:, None, :] == count
            pick_ref[c] = jnp.where(slot, 1.0, 0.0).reshape(slots, rows).astype(BF16)
            heavy = jnp.where(slot, weight[:, None, :], 0.0).reshape(slots, rows).astype(BF16)
            weigh_ref[c] = lax.dot_general(
                eye, heavy, (((1,), (1,)), ((), ())), preferred_element_type=F32
            ).astype(BF16)

    arrived(5)
    tables()
    arrived(0)
    arrived(2)
    arrived(1)
    arrived(3)
    lower = 2 * me < n
    pl.when(lower)(lambda: attend(blocks))
    pl.when(jnp.logical_not(lower))(lambda: attend(blocks[::-1]))

    wide = out_w.shape[1]
    tile = min(512, wide)

    def project(j, part_ref, at):
        for start in range(0, wide, tile):
            cols = slice(start, start + tile)
            more = jnp.dot(
                part_ref, out_w[pl.ds(pl.multiple_of(j * lw, 128), lw), cols], preferred_element_type=F32
            )
            mixed_ref[:, cols] = at[:, cols].astype(F32) + more

    weights.wait()
    project(me, obuf[me], res_ref)
    for d in range(1, n):
        j = lax.rem(me + d, n)
        here = pl.ds(pl.multiple_of(j * lw, 128), lw)
        remote(obuf.at[j], out_ref.at[:, here], osend.at[j], orecv.at[j], (j, dp)).wait_recv()
        project(j, out_ref[:, here], mixed_ref)
    square = jnp.zeros((rows, 1), F32)
    for start in range(0, wide, tile):
        chunk = mixed_ref[:, start : start + tile]
        square = square + jnp.sum(chunk * chunk, axis=-1, keepdims=True)
    factor = lax.rsqrt(square * (1.0 / wide) + 1e-06)
    for start in range(0, wide, tile):
        cols = slice(start, start + tile)
        normed_ref[:, cols] = (mixed_ref[:, cols] * factor * ngain_ref[:, cols]).astype(BF16)

    def finish():
        for copy in sends:
            copy.wait_send()
        for d in range(1, n):
            j = lax.rem(me + d, n)
            here = pl.ds(pl.multiple_of(j * lw, 128), lw)
            remote(obuf.at[j], out_ref.at[:, here], osend.at[j], orecv.at[j], (j, dp)).wait_send()

    return finish


class Place:
    def __init__(self, outer, inner, ndp):
        self.outer, self.inner, self.ndp = outer, inner, ndp
        self.plane = inner * ndp
        sp, self.dp = lax.axis_index("sp"), lax.axis_index("dp")
        self.z, self.y = sp // inner, lax.rem(sp, inner)
        self.me = self.y * ndp + self.dp

    def along(self, z):
        return (z * self.inner + self.y, self.dp)

    def across(self, p):
        return (self.z * self.inner + p // self.ndp, lax.rem(p, self.ndp))

    def order(self):
        tables = [
            sorted(range(self.outer), key=lambda c: (abs(c - z), c if 2 * z < self.outer else -c))
            for z in range(self.outer)
        ]
        steps = []
        for s in range(self.outer):
            value = jnp.int32(tables[0][s])
            for z in range(1, self.outer):
                value = jnp.where(self.z == z, tables[z][s], value)
            steps.append(value)
        return steps

    def relays(self):
        top = self.outer - 1
        tables = []
        for z in range(self.outer):
            late = lambda c, z=z: c + z if c > z else (top - c) + (top - z)
            tables.append(sorted([c for c in range(self.outer) if c != z], key=late))
        steps = []
        for s in range(top):
            value = jnp.int32(tables[0][s])
            for z in range(1, self.outer):
                value = jnp.where(self.z == z, tables[z][s], value)
            steps.append(value)
        return steps


def moe_kernel(
    outer, inner, ndp, parts, lots, x_ref, pick_ref, weigh_ref, mixed_ref, gate_hbm, up_hbm, down_hbm, out_ref, pair_w,
    gath, staged, recv, hidden, eout, back, from_below, from_above, partial, mine, down_w,
    wsem, gsend, grecv, psend, precv, bsend, brecv, ssend, srecv,
):
    at = Place(outer, inner, ndp)
    z, plane = at.z, at.plane
    block, width = recv.shape[2], recv.shape[3]
    held, ff, _ = down_w.shape
    cap = block // held
    piece = width // parts
    spans = [slice(h * piece, (h + 1) * piece) for h in range(parts)]
    lot = width // lots
    wide = [slice(g * lot, (g + 1) * lot) for g in range(lots)]
    ratio = parts // lots
    order = at.order()
    edge = (z == 0) | (z == outer - 1)
    gate_w, up_w = pair_w.at[:, :width, :ff], pair_w.at[:, :width, ff : 2 * ff]
    loads = [
        pltpu.make_async_copy(a, b, wsem.at[i])
        for i, (a, b) in enumerate(((gate_hbm, gate_w), (up_hbm, up_w), (down_hbm, down_w)))
    ]
    for load in loads:
        load.start()

    def slab(ref, c, h):
        return ref.at[c, :, spans[h]]

    def up(c, h, src=None):
        return remote(
            slab(gath, c, h) if src is None else src, slab(gath, c, h), gsend.at[0, c, h], grecv.at[c, h],
            at.along(jnp.minimum(z + 1, outer - 1)),
        )

    def down(c, h, src=None):
        return remote(
            slab(gath, c, h) if src is None else src, slab(gath, c, h), gsend.at[1, c, h], grecv.at[c, h],
            at.along(jnp.maximum(z - 1, 0)),
        )

    def other(d):
        return lax.rem(at.me + d, plane)

    def out_to(c, d, g):
        p = other(d)
        return remote(
            staged.at[c, p, :, wide[g]], recv.at[c, at.me, :, wide[g]],
            psend.at[c, p, g], precv.at[c, at.me, g], at.across(p),
        )

    def back_to(c, d, g):
        p = other(d)
        return remote(
            eout.at[c, p, :, wide[g]], back.at[c, at.me, :, wide[g]],
            bsend.at[c, p, g], brecv.at[c, at.me, g], at.across(p),
        )

    def chosen(step):
        c = order[0]
        for i in range(1, outer):
            c = jnp.where(step == i, order[i], c)
        return c

    def hand_on(c, h, src=None):
        @pl.when((c <= z) & (z < outer - 1))
        def _():
            up(c, h, src).start()

        @pl.when((c >= z) & (z > 0))
        def _():
            down(c, h, src).start()

    def sort_out(c, g, rows):
        for p in range(plane):
            staged[c, p, :, wide[g]] = jnp.dot(
                pick_ref[c, p * block : (p + 1) * block, :], rows, preferred_element_type=F32
            ).astype(BF16)

    def give(c, g):
        for d in range(1, plane):
            out_to(c, d, g).start()
        recv[c, at.me, :, wide[g]] = staged[c, at.me, :, wide[g]]

    def spread(step):
        sides = ((z - step, z >= step), (z + step, z + step < outer))
        for h in range(parts):
            for c, there in sides:

                @pl.when(there)
                def _(c=c, h=h):
                    remote(
                        slab(gath, c, h), slab(gath, c, h), gsend.at[0, c, h], grecv.at[c, h], at.along(c)
                    ).wait_recv()
                    hand_on(c, h)

            for c, there in sides if (h + 1) % ratio == 0 else ():

                @pl.when(there)
                def _(c=c, g=h // ratio):
                    sort_out(c, g, gath[c, :, wide[g]])
                    give(c, g)

    def give_back(c, g):
        for d in range(1, plane):
            back_to(c, d, g).start()

    def work(step):
        c = chosen(step)
        for d in range(1, plane):
            p = other(d)
            for g in range(lots):
                remote(
                    staged.at[c, p, :, wide[g]], recv.at[c, p, :, wide[g]],
                    psend.at[c, p, g], precv.at[c, p, g], at.across(p),
                ).wait_recv()

        @pl.when(step == 0)
        def _():
            for load in loads:
                load.wait()

        tile = min(512, ff)
        for e in range(held):
            rows = recv[c, :, e * cap : (e + 1) * cap, :].reshape(plane * cap, width)
            for start in range(0, ff, tile):
                cols = slice(start, start + tile)
                gate = jnp.dot(rows, pair_w[e, :width, start : start + tile], preferred_element_type=F32)
                upper = jnp.dot(rows, pair_w[e, :width, ff + start : ff + start + tile], preferred_element_type=F32)
                clamped = jnp.minimum(gate, 7.0)
                hidden[e, :, cols] = (
                    (jnp.clip(upper, -7.0, 7.0) + 1.0) * clamped * jax.nn.sigmoid(1.702 * clamped)
                ).astype(BF16)
        tile = min(512, piece)
        for g in range(lots):
            for e in range(held):
                for start in range(g * lot, (g + 1) * lot, tile):
                    cols = slice(start, start + tile)
                    result = jnp.dot(hidden[e], down_w[e, :, cols], preferred_element_type=F32).astype(BF16)
                    eout[c, :, e * cap : (e + 1) * cap, cols] = result.reshape(plane, cap, tile)
            back[c, at.me, :, wide[g]] = eout[c, at.me, :, wide[g]]

            @pl.when((step > 0) & ((step > 1) | jnp.logical_not(edge)))
            def _(g=g):
                give_back(c, g)

    def rise(c, h):
        return remote(
            slab(partial, c, h), slab(from_below, c, h), ssend.at[c, h], srecv.at[0, c, h],
            at.along(jnp.minimum(z + 1, outer - 1)),
        )

    def fall(c, h):
        return remote(
            slab(partial, c, h), slab(from_above, c, h), ssend.at[c, h], srecv.at[1, c, h],
            at.along(jnp.maximum(z - 1, 0)),
        )

    def pass_on(c, h):
        @pl.when(c > z)
        def _():
            rise(c, h).start()

        @pl.when(c < z)
        def _():
            fall(c, h).start()

    def first(c):
        return ((c > z) & (z == 0)) | ((c < z) & (z == outer - 1))

    tile = min(512, piece)

    def collect(step, h):
        c = chosen(step)
        g = h // ratio
        for d in range(1, plane) if h % ratio == 0 else ():
            p = other(d)
            remote(
                eout.at[c, p, :, wide[g]], back.at[c, p, :, wide[g]],
                bsend.at[c, p, g], brecv.at[c, p, g], at.across(p),
            ).wait_recv()
        for start in range(h * piece, (h + 1) * piece, tile):
            cols = slice(start, start + tile)
            total = jnp.dot(
                weigh_ref[c], back[c, :, :, cols].reshape(plane * block, tile), preferred_element_type=F32
            )
            mine[c, :, cols] = total
            partial[c, :, cols] = total.astype(BF16)

        @pl.when(first(c))
        def _():
            pass_on(c, h)

    def relay(c, h):
        @pl.when(jnp.logical_not(first(c)))
        def _():
            for side, (here, source) in enumerate(((c > z, from_below), (c < z, from_above))):

                @pl.when(here)
                def _(side=side, source=source):
                    remote(
                        slab(partial, c, h), slab(source, c, h), ssend.at[c, h], srecv.at[side, c, h], at.along(c)
                    ).wait_recv()
                    for start in range(h * piece, (h + 1) * piece, tile):
                        cols = slice(start, start + tile)
                        partial[c, :, cols] = (mine[c, :, cols] + source[c, :, cols].astype(F32)).astype(BF16)

            pass_on(c, h)

    for h in range(parts):
        hand_on(z, h, x_ref.at[:, spans[h]])
    for g in range(lots):
        sort_out(z, g, x_ref[:, wide[g]])
        give(z, g)

    def turn(step, carry):
        @pl.when((step > 0) & (step < outer))
        def _():
            spread(step)

        @pl.when((step > 0) & (step <= outer))
        def _():
            work(step - 1)

        return carry

    lax.fori_loop(1, outer + 1, turn, 0)

    @pl.when(edge)
    def _():
        if outer > 1:
            for g in range(lots):
                give_back(order[1], g)

    for g in range(lots):
        give_back(z, g)

    relays = at.relays()
    early = outer - 2 if outer == 4 else 0
    for k in range(outer - 1):
        step = jnp.where(edge, k + 2 if k < outer - 2 else 1, k + 1)
        for h in range(parts):
            collect(step, h)
            if 0 < k <= early:
                relay(relays[k - 1], h)
    for c in relays[early:]:
        for h in range(parts):
            relay(c, h)
    for h in range(parts):
        collect(0, h)
    for h in range(parts):
        @pl.when(z > 0)
        def _(h=h):
            remote(
                slab(partial, z, h), slab(from_below, z, h), ssend.at[z, h], srecv.at[0, z, h],
                at.along(jnp.maximum(z - 1, 0)),
            ).wait_recv()

        @pl.when(z < outer - 1)
        def _(h=h):
            remote(
                slab(partial, z, h), slab(from_above, z, h), ssend.at[z, h], srecv.at[1, z, h],
                at.along(jnp.minimum(z + 1, outer - 1)),
            ).wait_recv()

        for start in range(h * piece, (h + 1) * piece, tile):
            cols = slice(start, start + tile)
            total = mine[z, :, cols] + mixed_ref[:, cols]
            total = total + jnp.where(z > 0, from_below[z, :, cols].astype(F32), 0.0)
            total = total + jnp.where(z < outer - 1, from_above[z, :, cols].astype(F32), 0.0)
            out_ref[:, cols] = total.astype(BF16)

    for step, c in enumerate(order):
        for h in range(parts):

            @pl.when((c <= z) & (z < outer - 1))
            def _(c=c, h=h):
                up(c, h).wait_send()

            @pl.when((c >= z) & (z > 0))
            def _(c=c, h=h):
                down(c, h).wait_send()

            if step > 0:
                rise(c, h).wait_send()
        for g in range(lots):
            for d in range(1, plane):
                out_to(c, d, g).wait_send()
                back_to(c, d, g).wait_send()


def layer_kernel(n, outer, held, rows, heads_local, hd, hv, sliced, parts, lots, count, *refs):
    small, (gate, up, down), (out,) = refs[:12], refs[12:15], refs[15:16]
    normed, mixed, pick, weigh, pair_w = refs[16:21]
    first, rest = refs[21 : 21 + count], refs[21 + count :]
    wide = out.shape[1]
    finish = attention_kernel(
        n, outer, held, rows, heads_local, hd, hv, sliced, *small,
        normed, mixed, pick, weigh, pair_w.at[0, : n * heads_local * hv, :wide], *first,
    )
    moe_kernel(
        outer, n // outer, lax.axis_size("dp"), parts, lots, normed, pick, weigh, mixed, gate, up, down, out, pair_w, *rest
    )
    finish()


def layer(
    n, outer, capacity, q1, k1, q2, k2, vv, lam, gain, routes, rw, residual, ngain, out_weight,
    gate_weight, up_weight, down_weight,
):
    rows, width = residual.shape
    heads, topk = lam.shape[0], routes.shape[0]
    heads_local = heads // n
    hd = q1.shape[1] // heads
    hv = vv.shape[1] // heads
    held, _, ff = gate_weight.shape
    plane = n // outer * lax.axis_size("dp")
    block = held * capacity
    parts = 4 if width % 512 == 0 else 1
    lots = 2 if parts > 1 else 1
    arrays, sliced = [], []
    for array, each in ((q1, hd), (k1, hd), (q2, hd), (k2, hd), (vv, hv)):
        w = each * heads_local
        good = w % 128 == 0
        arrays.append(array if good else array.reshape(rows, n, w).transpose(1, 0, 2))
        sliced.append(good)
    w, lw = hd * heads_local, hv * heads_local
    group = 2 if n % 2 == 0 else 1
    flat = (outer, plane, block, width)
    line = (outer, rows, width)
    dma = pltpu.SemaphoreType.DMA
    shared = [
        VMEM((rows, width), BF16),
        VMEM((rows, width), F32),
        VMEM((outer, plane * block, rows), BF16),
        VMEM((outer, rows, plane * block), BF16),
        VMEM((held, max(width, n * lw), max(2 * ff, width)), BF16),
    ]
    first = [VMEM((n, rows, w), BF16)] * 4 + [VMEM((n, rows, lw), BF16)] * 2
    first += [
        VMEM((group * rows, n * rows), F32),
        VMEM((heads_local, n * rows, n * rows), BF16),
        VMEM((rows, n * lw), BF16),
        VMEM((2 * topk, rows), F32),
        VMEM((n, 2 * topk, rows), F32),
        dma((6, n)),
        dma((6, n)),
        dma((6,)),
        dma((n,)),
        dma((n,)),
        dma,
    ]
    second = [
        VMEM(line, BF16),
        VMEM(flat, BF16),
        VMEM(flat, BF16),
        VMEM((held, plane * capacity, ff), BF16),
        VMEM(flat, BF16),
        VMEM(flat, BF16),
        VMEM(line, BF16),
        VMEM(line, BF16),
        VMEM(line, BF16),
        VMEM(line, F32),
        VMEM(down_weight.shape, BF16),
        dma((3,)),
        dma((2, outer, parts)),
        dma((outer, parts)),
        dma((outer, plane, lots)),
        dma((outer, plane, lots)),
        dma((outer, plane, lots)),
        dma((outer, plane, lots)),
        dma((outer, parts)),
        dma((2, outer, parts)),
    ]
    order = (1, 3, 0, 2, 4)
    return pl.pallas_call(
        functools.partial(
            layer_kernel, n, outer, held, rows, heads_local, hd, hv, [sliced[i] for i in order], parts, lots, len(first)
        ),
        out_shape=jax.ShapeDtypeStruct((rows, width), BF16),
        in_specs=[pl.BlockSpec(memory_space=pltpu.SMEM)] + vspec(5) + [pl.BlockSpec(memory_space=pl.ANY)] * 9,
        out_specs=vspec(1)[0],
        scratch_shapes=shared + first + second,
        compiler_params=pltpu.CompilerParams(
            collective_id=0, has_side_effects=True, vmem_limit_bytes=63 << 20
        ),
    )(lam, gain, routes, rw, residual, ngain, *arrays, out_weight, gate_weight, up_weight, down_weight)


def on_device(
    query_first,
    key_first,
    query_second,
    key_second,
    value_rows,
    mix_lambda,
    head_gain,
    residual,
    out_weight,
    norm_gain,
    routes,
    route_weights,
    gate_weight,
    up_weight,
    down_weight,
):
    n, ndp = lax.axis_size("sp"), lax.axis_size("dp")
    rows = query_first.shape[1]
    topk = routes.shape[2]
    held = gate_weight.shape[0]
    outer = 1
    while outer * outer < n:
        outer *= 2
    experts_all = held * n * ndp
    capacity = max(2, 3 * rows * topk // (2 * experts_all))
    capacity = -(-capacity // 8) * 8
    return layer(
        n, outer, capacity, query_first[0], key_first[0], query_second[0], key_second[0], value_rows[0],
        mix_lambda, head_gain[None, :], routes[0].T, route_weights[0].T, residual[0], norm_gain[None, :], out_weight,
        gate_weight, up_weight, down_weight,
    )[None]


def solution(mesh):
    spread = P("dp", "sp", None)
    split = P(("sp", "dp"), None, None)
    return jax.shard_map(
        on_device,
        mesh=mesh,
        in_specs=(spread,) * 5 + (P(), P(), spread, P(), P(), spread, spread) + (split,) * 3,
        out_specs=spread,
        check_vma=False,
    )
```
